32 devices in a mesh: sp: 8 (over z, y), tp: 4 (over x, core).
Axes of the slice: x: 2, y: 2, z: 4, core: 2. Of those that a mesh axis runs over, the one named last changes fastest.
Arguments:
- latents: bfloat16 [2048, 4096], P('sp'), may hold values from -0.4375 to 0.4375
- query_heads: bfloat16 [2048, 16, 128], P('sp', 'tp'), may hold values from -8 to 8
- key_heads: bfloat16 [2048, 16, 128], P('sp', 'tp'), may hold values from -8 to 8
- value_heads: bfloat16 [2048, 16, 128], P('sp', 'tp'), may hold values from -6 to 6
- map_outputs: bfloat16 [2048, 2, 16, 128], P('sp', None, 'tp'), may hold values from -6 to 6
- log_sums: float32 [2048, 16, 2], P('sp', 'tp'), may hold values from -600 to 600, as said below
- out_grad: bfloat16 [2048, 16, 128], P('sp', 'tp'), may hold values from -6 to 6
- mix_lambda: float32 [16], P('tp'), may hold values from 0.3 to 0.8
- norm_gain: float32 [128], replicated, may hold values from 0.1 to 1.9
Outputs:
- query_grad: bfloat16 [2048, 16, 128], P('sp', 'tp')
- key_grad: bfloat16 [2048, 16, 128], P('sp', 'tp')
- value_grad: bfloat16 [2048, 16, 128], P('sp', 'tp')
- weight_grad: float32 [4096, 2048], P('sp', 'tp')
The draws below stay inside these ranges and needn't reach their ends.
Inputs may be any that keep to these rules, and one draw needn't show every extreme that they name: query_heads, key_heads and value_heads together with map_outputs and log_sums are one consistent causal forward pass: log_sums is the row's log-sum of exp(score_m) over keys at or before the row, and map_outputs[:, m] is prob_m times value_heads rounded to bfloat16.
All inputs are finite; a program needn't handle non-finite values.
Results may differ from the reference program's by a relative error of at most 0.019.
Values may be sent and summed in bfloat16 or wider, within the bound.
A program may use at most 64 MiB of HBM per device.

```python
import math
import jax
import jax.numpy as jnp
from jax import lax

D = 4096
HEADS = 16
DH = 64
TOKENS = 2048


def attention_forward(key):
    shape = (TOKENS, HEADS, 2 * DH)
    query_f = jnp.clip(1.3 * jax.random.normal(jax.random.fold_in(key, 101), shape, jnp.float32), -8.0, 8.0)
    key_f = jnp.clip(1.3 * jax.random.normal(jax.random.fold_in(key, 102), shape, jnp.float32), -8.0, 8.0)
    value_f = jnp.clip(jax.random.normal(jax.random.fold_in(key, 103), shape, jnp.float32), -6.0, 6.0)
    query_low = query_f.astype(jnp.bfloat16)
    key_low = key_f.astype(jnp.bfloat16)
    value_low = value_f.astype(jnp.bfloat16)
    length = TOKENS
    span = math.gcd(length, 512)
    score_scale = DH ** (-0.5)

    def per_head(inputs):
        query_one, key_one, value_one = inputs
        query_split = query_one.astype(jnp.float32).reshape(length, 2, DH)
        key_split = key_one.astype(jnp.float32).reshape(length, 2, DH)
        value_wide = value_one.astype(jnp.float32)
        key_pos = jnp.arange(length, dtype=jnp.int32)

        def visit(block_index):
            anchor = (block_index * span).astype(jnp.int32)
            query_blk = lax.dynamic_slice_in_dim(query_split, anchor, span, 0)
            scores = jnp.einsum('qmd,kmd->mqk', query_blk, key_split) * score_scale
            query_pos = anchor + jnp.arange(span, dtype=jnp.int32)
            causal = key_pos[None, :] <= query_pos[:, None]
            masked = jnp.where(causal[None], scores, -jnp.inf)
            highest = jnp.max(masked, axis=-1, keepdims=True)
            log_total = highest + jnp.log(jnp.sum(jnp.exp(masked - highest), axis=-1, keepdims=True))
            probs = jnp.exp(masked - log_total)
            outputs = jnp.einsum('mqk,ke->mqe', probs, value_wide)
            return (log_total[..., 0].T, outputs)
        lse_blocks, out_blocks = lax.map(visit, jnp.arange(length // span, dtype=jnp.int32))
        lse_head = lse_blocks.reshape(length, 2)
        out_head = jnp.transpose(out_blocks, (1, 0, 2, 3)).reshape(2, length, 2 * DH)
        return (lse_head, out_head)
    lse_all, out_all = lax.map(per_head, (jnp.transpose(query_low, (1, 0, 2)), jnp.transpose(key_low, (1, 0, 2)), jnp.transpose(value_low, (1, 0, 2))))
    log_table = jnp.transpose(lse_all, (1, 0, 2))
    out_table = jnp.transpose(out_all, (2, 1, 0, 3)).astype(jnp.bfloat16)
    return (query_low, key_low, value_low, out_table, log_table)


def draw_query_heads(key, part):
    return attention_forward(key)[0]


def draw_key_heads(key, part):
    return attention_forward(key)[1]


def draw_value_heads(key, part):
    return attention_forward(key)[2]


def draw_map_outputs(key, part):
    return attention_forward(key)[3]


def draw_log_sums(key, part):
    return attention_forward(key)[4]


def raised(values, stream_key, source, target, parts, factor):
    def block_of(position):
        return (jnp.arange(values.shape[position]) // (values.shape[position] // parts)).reshape((-1,) + (1,) * (values.ndim - 1 - position))

    near = jax.random.permutation(stream_key, parts)[block_of(target)]
    far = (block_of(target) + parts // 2) % parts
    return jnp.where((block_of(source) == near) | (block_of(source) == far), factor * values, values)


def level_of(key, extent, split, least, top_value):
    factor_of, own = 1.0, jax.random.fold_in(key, 6)
    for position, shards_of in split:
        steps = jnp.exp(jax.random.uniform(jax.random.fold_in(own, position), (shards_of,), jnp.float32, least / len(split), top_value / len(split)))
        factor_of = factor_of * jnp.repeat(steps, extent[position] // shards_of).reshape([-1 if axis == position else 1 for axis in range(len(extent))])
    return factor_of


def noise(key, dims, scale, most, pieces=(), kind=jnp.bfloat16):
    level = level_of(key, dims, pieces, -0.22, 0.18) if pieces else 1.0
    values = jax.random.normal(key, dims, jnp.float32) * scale * level
    return jnp.minimum(jnp.maximum(values, -most), most).astype(kind)


def gaussian_with(stream_key, shape, deviation, reach, shards, heavy, kind=jnp.bfloat16):
    entries = deviation * jax.random.normal(stream_key, shape, jnp.float32)
    if shards:
        entries = entries * level_of(stream_key, shape, shards, -0.22, 0.18)
    return jnp.clip(raised(entries, jax.random.fold_in(stream_key, 3), *heavy), -reach, reach).astype(kind)


def setup_inputs(seed: int = 0) -> dict:
    seeds = jax.random.split(jax.random.key(seed), 10)
    return {
        "latents": gaussian_with(seeds[0], (TOKENS, D), 0.02, 0.4375, ((0, 8),), (0, 1, 8, 2.0)),
        "query_heads": draw_query_heads(jax.random.fold_in(seeds[9], 71), 0),
        "key_heads": draw_key_heads(jax.random.fold_in(seeds[9], 71), 0),
        "value_heads": draw_value_heads(jax.random.fold_in(seeds[9], 71), 0),
        "map_outputs": draw_map_outputs(jax.random.fold_in(seeds[9], 71), 0),
        "log_sums": draw_log_sums(jax.random.fold_in(seeds[9], 71), 0),
        "out_grad": noise(seeds[6], (TOKENS, HEADS, 2 * DH), 1.0, 6.0, ((0, 8), (1, 4))),
        "mix_lambda": jnp.clip(0.3 + 0.5 * jax.random.uniform(seeds[7], (HEADS,), jnp.float32) ** level_of(seeds[7], (HEADS,), ((0, 4),), -0.2, 0.2), 0.3, 0.8),
        "norm_gain": jnp.clip(1.0 + 0.18 * jax.random.normal(seeds[8], (2 * DH,), jnp.float32), 0.1, 1.9),
    }


EPSILON = 1e-05

def reference(latents, query_heads, key_heads, value_heads, map_outputs, log_sums, out_grad, mix_lambda, norm_gain):
    highest = lax.Precision.HIGHEST
    score_scale = DH ** (-0.5)
    first_map = map_outputs[:, 0].astype(jnp.float32)
    second_map = map_outputs[:, 1].astype(jnp.float32)
    lambda_col = mix_lambda[None, :, None]
    combined = first_map - lambda_col * second_map
    inverse = lax.rsqrt(lax.optimization_barrier(jnp.mean(combined * combined, axis=-1, keepdims=True)) + EPSILON)
    weighted = norm_gain[None, None, :] * out_grad.astype(jnp.float32)
    grad_out = (inverse * weighted - inverse ** 3 * combined * lax.optimization_barrier(jnp.mean(combined * weighted, axis=-1, keepdims=True))).astype(jnp.bfloat16)
    grad_wide = lax.optimization_barrier(grad_out).astype(jnp.float32)
    row_terms = jnp.stack([lax.optimization_barrier(jnp.sum(grad_wide * first_map, axis=-1)), lax.optimization_barrier(jnp.sum(grad_wide * second_map, axis=-1))], axis=-1)
    length = query_heads.shape[0]
    span = math.gcd(length, 512)

    def per_head(inputs):
        query_one, key_one, value_one, grad_one, lse_one, term_one, lam = inputs
        query_split = query_one.astype(jnp.float32).reshape(length, 2, DH)
        key_split = key_one.astype(jnp.float32).reshape(length, 2, DH)
        value_wide = value_one.astype(jnp.float32)
        grad_full = grad_one.astype(jnp.float32)
        key_pos = jnp.arange(length, dtype=jnp.int32)
        map_signs = jnp.stack([jnp.ones((), jnp.float32), -lam])

        def visit(running, block_index):
            key_acc, value_acc = running
            anchor = (block_index * span).astype(jnp.int32)
            query_blk = lax.dynamic_slice_in_dim(query_split, anchor, span, 0)
            grad_blk = lax.dynamic_slice_in_dim(grad_full, anchor, span, 0)
            lse_blk = lax.dynamic_slice_in_dim(lse_one, anchor, span, 0)
            term_blk = lax.dynamic_slice_in_dim(term_one, anchor, span, 0)
            scores = jnp.einsum('qmd,kmd->mqk', query_blk, key_split, precision=highest) * score_scale
            query_pos = anchor + jnp.arange(span, dtype=jnp.int32)
            causal = key_pos[None, :] <= query_pos[:, None]
            softmax_maps = jnp.exp(jnp.where(causal[None], scores - lse_blk.T[:, :, None], -jnp.inf))
            mixed_grad = jnp.dot(grad_blk, value_wide.T, precision=highest)
            score_grad = map_signs[:, None, None] * softmax_maps * (mixed_grad[None] - term_blk.T[:, :, None])
            score_low = lax.optimization_barrier(score_grad.astype(jnp.bfloat16)).astype(jnp.float32)
            diff_weights = lax.optimization_barrier((softmax_maps[0] - lam * softmax_maps[1]).astype(jnp.bfloat16)).astype(jnp.float32)
            value_acc = value_acc + jnp.dot(diff_weights.T, grad_blk, precision=highest)
            query_part = score_scale * jnp.einsum('mqk,kmd->qmd', score_low, key_split, precision=highest)
            key_acc = key_acc + score_scale * jnp.einsum('mqk,qmd->kmd', score_low, query_blk, precision=highest)
            return ((key_acc, value_acc), query_part)
        start_state = (jnp.zeros((length, 2, DH), jnp.float32), jnp.zeros((length, 2 * DH), jnp.float32))
        (key_acc, value_acc), query_parts = lax.scan(visit, start_state, jnp.arange(length // span, dtype=jnp.int32))
        return (query_parts.reshape(length, 2 * DH), key_acc.reshape(length, 2 * DH), value_acc)

    def head_major(array):
        return jnp.transpose(array, (1, 0, 2))
    query_all, key_all, value_all = lax.map(per_head, (head_major(query_heads), head_major(key_heads), head_major(value_heads), head_major(grad_out), head_major(log_sums), head_major(row_terms), mix_lambda))
    query_grad = head_major(query_all).astype(jnp.bfloat16)
    key_grad = head_major(key_all).astype(jnp.bfloat16)
    value_grad = head_major(value_all).astype(jnp.bfloat16)
    weight_grad = jnp.dot(latents.T, query_grad.reshape(length, -1), preferred_element_type=jnp.float32)
    return (query_grad, key_grad, value_grad, weight_grad)
```

```python
import functools
import math

import jax
import jax.numpy as jnp
from jax import lax
from jax.experimental import pallas as pl
from jax.experimental.pallas import tpu as pltpu
from jax.sharding import PartitionSpec as P

EPSILON = 1e-05
LOG2E = math.log2(math.e)
F32 = jnp.float32
BF16 = jnp.bfloat16
MESH = pl.DeviceIdType.MESH


def dot_nn(a, b):
    return lax.dot_general(a, b, (((1,), (0,)), ((), ())), preferred_element_type=F32)


def dot_nt(a, b):
    return lax.dot_general(a, b, (((1,), (1,)), ((), ())), preferred_element_type=F32)


def dot_tn(a, b):
    return lax.dot_general(a, b, (((0,), (0,)), ((), ())), preferred_element_type=F32)


def prologue(heads, width, lam_ref, gain_ref, mo_ref, og_ref, lse_ref, q_ref, k_ref, v_ref,
             kv_ref, qg_ref, col_ref):
    kv_ref[0] = k_ref[...]
    kv_ref[1] = v_ref[...]
    qg_ref[0] = q_ref[...]
    for h in range(heads):
        at = slice(h * width, (h + 1) * width)
        first = mo_ref[:, at].astype(F32)
        second = mo_ref[:, heads * width + h * width : heads * width + (h + 1) * width].astype(F32)
        lam = lam_ref[h]
        combined = first - lam * second
        inverse = lax.rsqrt(jnp.mean(combined * combined, axis=-1, keepdims=True) + EPSILON)
        weighted = gain_ref[...] * og_ref[:, at].astype(F32)
        grad = (
            inverse * weighted
            - inverse**3 * combined * jnp.mean(combined * weighted, axis=-1, keepdims=True)
        ).astype(BF16)
        qg_ref[1, :, at] = grad
        wide = grad.astype(F32)
        lse = lse_ref[h] * LOG2E
        log_lam = jnp.log(jnp.full((1, 1), lam, F32)) * LOG2E
        col_ref[h, :, 0:1] = lse[:, 0:1]
        col_ref[h, :, 1:2] = lse[:, 1:2] - log_lam
        col_ref[h, :, 2:3] = jnp.sum(wide * first, axis=-1, keepdims=True)
        col_ref[h, :, 3:4] = jnp.sum(wide * second, axis=-1, keepdims=True)


def main_kernel(nsp, ntp, heads, width, lat, kv, qg, col, row,
                dq_out, dk_out, dv_out, wg_out,
                kvb, qgb, stb, dqb, latb, dq_acc, dk_acc, dv_acc,
                kv_s, qg_s, st_s, dq_s, kv_r, qg_r, st_r, dq_r,
                la_s, la_r, lb_s, lb_r, own_sem):
    nz = nsp // 2
    s = lax.axis_index("sp")
    t = lax.axis_index("tp")
    z, y = s // 2, lax.rem(s, 2)
    rows = kv.shape[1]
    part = rows // ntp
    slab = lat.shape[1] // nsp
    score_scale = (width // 2) ** (-0.5)
    exp_scale = score_scale * LOG2E

    barrier = pltpu.get_barrier_semaphore()
    for d in range(1, nsp):
        pl.semaphore_signal(barrier, inc=1, device_id={"sp": lax.rem(s + d, nsp)}, device_id_type=MESH)
    for d in range(1, ntp):
        pl.semaphore_signal(barrier, inc=1, device_id={"tp": lax.rem(t + d, ntp)}, device_id_type=MESH)
    pl.semaphore_wait(barrier, nsp - 1 + ntp - 1)

    def copy(src, dst, send, recv, to):
        return pltpu.make_async_remote_copy(
            src_ref=src, dst_ref=dst, send_sem=send, recv_sem=recv,
            device_id={"sp": to}, device_id_type=MESH)

    side = 2 * z + (1 - y)

    def kv_copy(block, lane, k, src=None):
        to = jnp.minimum(s + 2, nsp - 1) if lane == 0 else side
        return copy(kvb.at[block] if src is None else src, kvb.at[block],
                    kv_s.at[lane, k], kv_r.at[block], to)

    def qg_copies(block, lane, k, own=False):
        to = jnp.maximum(s - 2, 0) if lane == 0 else side
        return (
            copy(qg if own else qgb.at[block], qgb.at[block], qg_s.at[lane, k], qg_r.at[block], to),
            copy(row if own else stb.at[block], stb.at[block], st_s.at[lane, k], st_r.at[block], to),
        )

    @pl.when(z < nz - 1)
    def _():
        kv_copy(s, 0, 0, kv).start()

    @pl.when(z > 0)
    def _():
        for c in qg_copies(s, 0, 0, True):
            c.start()

    @pl.when(y == 0)
    def _():
        kv_copy(s, 1, 0, kv).start()

    @pl.when(y == 1)
    def _():
        for c in qg_copies(s, 1, 0, True):
            c.start()

    lane_id = lax.broadcasted_iota(jnp.int32, (1, width), 1)
    low = jnp.where(lane_id < width // 2, 1.0, 0.0).astype(BF16)
    high = jnp.where(lane_id < width // 2, 0.0, 1.0).astype(BF16)

    def split(x):
        return jnp.concatenate([x * low, x * high], axis=0)

    def query_side(kv_at, diagonal):
        def one(h, carry):
            at = pl.ds(pl.multiple_of(h * width, width), width)
            keys = split(kv_at[0, :, at])
            scores = dot_nt(qg[0, :, at], keys)
            mixed = dot_nt(qg[1, :, at], kv_at[1, :, at])
            stats = col[h]
            x1 = scores[:, :rows] * exp_scale - stats[:, 0:1]
            x2 = scores[:, rows:] * exp_scale - stats[:, 1:2]
            if diagonal:
                seen = (lax.broadcasted_iota(jnp.int32, (rows, rows), 1)
                        <= lax.broadcasted_iota(jnp.int32, (rows, rows), 0))
                x1 = jnp.where(seen, x1, -jnp.inf)
                x2 = jnp.where(seen, x2, -jnp.inf)
            g1 = (jnp.exp2(x1) * (mixed - stats[:, 2:3])).astype(BF16)
            g2 = (jnp.exp2(x2) * (stats[:, 3:4] - mixed)).astype(BF16)
            part_dq = dot_nn(jnp.concatenate([g1, g2], axis=1), keys)
            if diagonal:
                dq_acc[:, at] = part_dq
            else:
                dq_acc[:, at] += part_dq
            return carry
        lax.fori_loop(0, heads, one, 0)

    def key_side(qg_at, row_at, diagonal):
        def one(h, carry):
            at = pl.ds(pl.multiple_of(h * width, width), width)
            queries = split(qg_at[0, :, at])
            grads = qg_at[1, :, at]
            scores = dot_nt(kv[0, :, at], queries)
            mixed = dot_nt(kv[1, :, at], grads)
            stats = row_at[h]
            x1 = scores[:, :rows] * exp_scale - stats[0:1]
            x2 = scores[:, rows:] * exp_scale - stats[1:2]
            if diagonal:
                seen = (lax.broadcasted_iota(jnp.int32, (rows, rows), 0)
                        <= lax.broadcasted_iota(jnp.int32, (rows, rows), 1))
                x1 = jnp.where(seen, x1, -jnp.inf)
                x2 = jnp.where(seen, x2, -jnp.inf)
            p1 = jnp.exp2(x1)
            p2 = jnp.exp2(x2)
            g1 = (p1 * (mixed - stats[2:3])).astype(BF16)
            g2 = (p2 * (stats[3:4] - mixed)).astype(BF16)
            part_dv = dot_nn((p1 - p2).astype(BF16), grads)
            part_dk = dot_nn(jnp.concatenate([g1, g2], axis=1), queries)
            if diagonal:
                dv_acc[:, at] = part_dv
                dk_acc[:, at] = part_dk
            else:
                dv_acc[:, at] += part_dv
                dk_acc[:, at] += part_dk
            return carry
        lax.fori_loop(0, heads, one, 0)

    def lat_copy(d):
        to = lax.rem(s + d, nsp)
        mine = pl.ds(pl.multiple_of(t * part, part), part)
        return copy(lat.at[mine, pl.ds(pl.multiple_of(to * slab, slab), slab)],
                    latb.at[s, mine, :], la_s.at[d], la_r.at[d], to)

    def own_lat():
        return pltpu.make_async_copy(
            lat.at[pl.ds(pl.multiple_of(t * part, part), part), pl.ds(pl.multiple_of(s * slab, slab), slab)],
            latb.at[s, pl.ds(pl.multiple_of(t * part, part), part), :], own_sem)

    def share_copy(d):
        mine = pl.ds(pl.multiple_of(t * part, part), part)
        return pltpu.make_async_remote_copy(
            src_ref=latb.at[:, mine, :], dst_ref=latb.at[:, mine, :],
            send_sem=lb_s.at[d], recv_sem=lb_r.at[d],
            device_id={"tp": lax.rem(t + d, ntp)}, device_id_type=MESH)

    own_lat().start()
    query_side(kv, True)
    key_side(qg, row, True)
    for d in range(1, nsp):
        lat_copy(d).start()

    def step(k, carry):
        below, above = z - k, z + k
        has_below, has_above = below >= 0, above < nz
        kb = jnp.maximum(below, 0) * 2 + y
        qb = jnp.minimum(above, nz - 1) * 2 + y

        @pl.when(has_below)
        def _():
            kv_copy(kb, 0, 0).wait_recv()
            kv_copy(kb, 1, k).start()

        @pl.when(has_below & (z < nz - 1))
        def _():
            kv_copy(kb, 0, k).start()

        @pl.when(has_above)
        def _():
            for c in qg_copies(qb, 0, 0):
                c.wait_recv()
            for c in qg_copies(qb, 1, k):
                c.start()

        @pl.when(has_above & (z > 0))
        def _():
            for c in qg_copies(qb, 0, k):
                c.start()

        def turn(c, carry):
            dist = k - c
            other = jnp.where(c == 0, y, 1 - y)
            bz, qz = z - dist, z + dist
            use_kv = (bz >= 0) & (dist < nz) & ((dist > 0) | (y == 1))
            use_qg = (qz < nz) & (dist < nz) & ((dist > 0) | (y == 0))
            kblk = jnp.maximum(bz, 0) * 2 + other
            qblk = jnp.minimum(qz, nz - 1) * 2 + other

            @pl.when(use_kv)
            def _():
                @pl.when(c == 1)
                def _():
                    kv_copy(kblk, 1, 0).wait_recv()
                query_side(kvb.at[kblk], False)

            @pl.when(use_qg)
            def _():
                @pl.when(c == 1)
                def _():
                    for w in qg_copies(qblk, 1, 0):
                        w.wait_recv()
                key_side(qgb.at[qblk], stb.at[qblk], False)
            return carry
        lax.fori_loop(0, 2, turn, 0)
        return carry

    lax.fori_loop(1, nz + 1, step, 0)

    dq_out[...] = (dq_acc[...] * score_scale).astype(BF16)

    def dq_copy(block, lane, idx, src=None):
        to = (jnp.minimum(s + 2, nsp - 2 + y), jnp.maximum(s - 2, y), side)[lane]
        return copy(dqb.at[block] if src is None else src, dqb.at[block],
                    dq_s.at[lane, idx], dq_r.at[block], to)

    @pl.when(z < nz - 1)
    def _():
        dq_copy(s, 0, z, dq_out).start()

    @pl.when(z > 0)
    def _():
        dq_copy(s, 1, z, dq_out).start()

    dq_copy(s, 2, z, dq_out).start()

    dk_out[...] = (dk_acc[...] * score_scale).astype(BF16)
    dv_out[...] = dv_acc[...].astype(BF16)

    own_lat().wait()
    for d in range(1, nsp):
        lat_copy(d).wait_recv()
    for d in range(1, ntp):
        share_copy(d).start()
    for d in range(1, ntp):
        share_copy(d).wait_recv()

    wg_out[...] = dot_tn(latb[s], dq_out[...])

    def add_block(block):
        wg_out[...] += dot_tn(latb[block], dqb[block])

    def gather(k, carry):
        for lane, there, ok, more in (
            (0, z - k, z - k >= 0, z < nz - 1),
            (1, z + k, z + k < nz, z > 0),
        ):
            bz = jnp.clip(there, 0, nz - 1)
            block = bz * 2 + y

            @pl.when(ok)
            def _():
                dq_copy(block, lane, bz).wait_recv()
                dq_copy(block, 2, bz).start()

            @pl.when(ok & more)
            def _():
                dq_copy(block, lane, bz).start()

        def turn(c, carry):
            dist = jnp.where(c < 2, k, k - 1)
            up = lax.rem(c, 2)
            bz = jnp.where(up == 0, z - dist, z + dist)
            ok = (bz >= 0) & (bz < nz) & (dist < nz) & ((dist > 0) | (up == 0))
            other = jnp.where(c < 2, y, 1 - y)
            block = jnp.clip(bz, 0, nz - 1) * 2 + other

            @pl.when(ok)
            def _():
                @pl.when(c >= 2)
                def _():
                    dq_copy(block, 2, 0).wait_recv()
                add_block(block)
            return carry
        lax.fori_loop(0, 4, turn, 0)
        return carry

    lax.fori_loop(1, nz + 1, gather, 0)

    def drain(k, carry):
        below, above = z - k, z + k
        has_below, has_above = below >= 0, above < nz

        @pl.when(has_below & (z < nz - 1))
        def _():
            kv_copy(s, 0, k).wait_send()

        @pl.when(has_below & ((k > 0) | (y == 0)))
        def _():
            kv_copy(s, 1, k).wait_send()

        @pl.when(has_above & (z > 0))
        def _():
            for c in qg_copies(s, 0, k):
                c.wait_send()

        @pl.when(has_above & ((k > 0) | (y == 1)))
        def _():
            for c in qg_copies(s, 1, k):
                c.wait_send()

        @pl.when((k <= z) & (z < nz - 1))
        def _():
            dq_copy(s, 0, k).wait_send()

        @pl.when((k >= z) & (z > 0))
        def _():
            dq_copy(s, 1, k).wait_send()

        dq_copy(s, 2, k).wait_send()
        return carry

    lax.fori_loop(0, nz, drain, 0)
    for d in range(1, nsp):
        lat_copy(d).wait_send()
    for d in range(1, ntp):
        share_copy(d).wait_send()


def vmem():
    return pl.BlockSpec(memory_space=pltpu.VMEM)


def body(nsp, ntp, latents, query_heads, key_heads, value_heads, map_outputs, log_sums, out_grad,
         mix_lambda, norm_gain):
    rows, heads, width = query_heads.shape
    flat = (rows, heads * width)
    kv, qg, col = pl.pallas_call(
        functools.partial(prologue, heads, width),
        out_shape=(
            jax.ShapeDtypeStruct((2,) + flat, BF16),
            jax.ShapeDtypeStruct((2,) + flat, BF16),
            jax.ShapeDtypeStruct((heads, rows, 4), F32),
        ),
        in_specs=[pl.BlockSpec(memory_space=pltpu.SMEM)] + [vmem()] * 7,
        out_specs=(vmem(),) * 3,
        name="prologue",
    )(
        mix_lambda,
        norm_gain[None, :],
        map_outputs.reshape(rows, 2 * heads * width),
        out_grad.reshape(flat),
        jnp.transpose(log_sums, (1, 0, 2)),
        query_heads.reshape(flat),
        key_heads.reshape(flat),
        value_heads.reshape(flat),
    )
    row = jnp.transpose(col, (0, 2, 1))
    slab = latents.shape[1] // nsp
    nz = nsp // 2
    dma = pltpu.SemaphoreType.DMA
    dq, dk, dv, wg = pl.pallas_call(
        functools.partial(main_kernel, nsp, ntp, heads, width),
        out_shape=(
            jax.ShapeDtypeStruct(flat, BF16),
            jax.ShapeDtypeStruct(flat, BF16),
            jax.ShapeDtypeStruct(flat, BF16),
            jax.ShapeDtypeStruct((slab, heads * width), F32),
        ),
        in_specs=[vmem()] * 5,
        out_specs=(vmem(),) * 4,
        scratch_shapes=[
            pltpu.VMEM((nsp, 2) + flat, BF16),
            pltpu.VMEM((nsp, 2) + flat, BF16),
            pltpu.VMEM((nsp, heads, 4, rows), F32),
            pltpu.VMEM((nsp,) + flat, BF16),
            pltpu.VMEM((nsp, rows, slab), BF16),
            pltpu.VMEM(flat, F32),
            pltpu.VMEM(flat, F32),
            pltpu.VMEM(flat, F32),
            dma((2, nz)), dma((2, nz)), dma((2, nz)), dma((3, nz)),
            dma((nsp,)), dma((nsp,)), dma((nsp,)), dma((nsp,)),
            dma((nsp,)), dma((nsp,)), dma((ntp,)), dma((ntp,)),
            dma,
        ],
        compiler_params=pltpu.CompilerParams(collective_id=0, has_side_effects=True),
        name="main",
    )(latents, kv, qg, col, row)
    shape = (rows, heads, width)
    return dq.reshape(shape), dk.reshape(shape), dv.reshape(shape), wg


def solution(mesh):
    placed = (
        P("sp", None),
        P("sp", "tp", None),
        P("sp", "tp", None),
        P("sp", "tp", None),
        P("sp", None, "tp", None),
        P("sp", "tp", None),
        P("sp", "tp", None),
        P("tp"),
        P(),
    )
    return jax.shard_map(
        functools.partial(body, mesh.shape["sp"], mesh.shape["tp"]),
        mesh=mesh,
        in_specs=placed,
        out_specs=(P("sp", "tp", None), P("sp", "tp", None), P("sp", "tp", None), P("sp", "tp")),
        check_vma=False,
    )
```

```python
import functools
import math

import jax
import jax.numpy as jnp
from jax import lax
from jax.experimental import pallas as pl
from jax.experimental.pallas import tpu as pltpu
from jax.sharding import PartitionSpec as P

EPSILON = 1e-05
LOG2E = math.log2(math.e)
F32 = jnp.float32
BF16 = jnp.bfloat16
MESH = pl.DeviceIdType.MESH


def dot_nn(a, b):
    return lax.dot_general(a, b, (((1,), (0,)), ((), ())), preferred_element_type=F32)


def dot_nt(a, b):
    return lax.dot_general(a, b, (((1,), (1,)), ((), ())), preferred_element_type=F32)


def dot_tn(a, b):
    return lax.dot_general(a, b, (((0,), (0,)), ((), ())), preferred_element_type=F32)


def norm_backward(heads, width, lam_ref, gain_ref, mo_ref, og_ref, lse_ref, grad_ref, col_ref, row_ref):
    for h in range(heads):
        first = mo_ref[:, 0, h, :].astype(F32)
        second = mo_ref[:, 1, h, :].astype(F32)
        lam = lam_ref[h]
        combined = first - lam * second
        inverse = lax.rsqrt(jnp.mean(combined * combined, axis=-1, keepdims=True) + EPSILON)
        weighted = gain_ref[...] * og_ref[:, h, :].astype(F32)
        grad = (
            inverse * weighted
            - inverse**3 * combined * jnp.mean(combined * weighted, axis=-1, keepdims=True)
        ).astype(BF16)
        grad_ref[:, h * width : (h + 1) * width] = grad
        wide = grad.astype(F32)
        lse = lse_ref[h] * LOG2E
        log_lam = jnp.log(jnp.full((1, 1), lam, F32)) * LOG2E
        lane = lax.broadcasted_iota(jnp.int32, wide.shape, 1)
        stats = jnp.where(lane == 0, lse[:, 0:1], lse[:, 1:2] - log_lam)
        stats = jnp.where(lane == 2, jnp.sum(wide * first, axis=-1, keepdims=True), stats)
        stats = jnp.where(lane == 3, jnp.sum(wide * second, axis=-1, keepdims=True), stats)
        col_ref[h] = stats
        row_ref[h] = jnp.transpose(stats)[0:4]


def main_kernel(nsp, ntp, heads, width, lam, gain, lat, own_k, own_v, own_q, mo, og, lse,
                dq_out, dk_out, dv_out, wg_out,
                own_g, col, row, own_dq, kvb, qgb, stb, dqb, latb, dq_acc, dk_acc, dv_acc,
                kv_s, qg_s, st_s, dq_s, kv_r, qg_r, st_r, dq_r,
                la_s, la_r, lb_s, lb_r, own_sem):
    nz = nsp // 2
    s = lax.axis_index("sp")
    t = lax.axis_index("tp")
    z, y = s // 2, lax.rem(s, 2)
    rows = own_k.shape[0]
    part = rows // ntp
    slab = lat.shape[1] // nsp
    score_scale = (width // 2) ** (-0.5)
    exp_scale = score_scale * LOG2E

    barrier = pltpu.get_barrier_semaphore()
    for d in range(1, nsp):
        pl.semaphore_signal(barrier, inc=1, device_id={"sp": lax.rem(s + d, nsp)}, device_id_type=MESH)
    for d in range(1, ntp):
        pl.semaphore_signal(barrier, inc=1, device_id={"tp": lax.rem(t + d, ntp)}, device_id_type=MESH)
    pl.semaphore_wait(barrier, nsp - 1 + ntp - 1)

    def copy(src, dst, send, recv, to):
        return pltpu.make_async_remote_copy(
            src_ref=src, dst_ref=dst, send_sem=send, recv_sem=recv,
            device_id={"sp": to}, device_id_type=MESH)

    side = 2 * z + (1 - y)

    def kv_copy(block, lane, k, p, src=None):
        to = jnp.minimum(s + 2, nsp - 1) if lane == 0 else side
        return copy(kvb.at[block, p] if src is None else src, kvb.at[block, p],
                    kv_s.at[lane, p, k], kv_r.at[p, block], to)

    def qg_copy(block, lane, k, p, src=None):
        to = jnp.maximum(s - 2, 0) if lane == 0 else side
        return copy(qgb.at[block, p] if src is None else src, qgb.at[block, p],
                    qg_s.at[lane, p, k], qg_r.at[p, block], to)

    def st_copy(block, lane, k, src=None):
        to = jnp.maximum(s - 2, 0) if lane == 0 else side
        return copy(stb.at[block] if src is None else src, stb.at[block],
                    st_s.at[lane, k], st_r.at[block], to)

    for p, src in ((0, own_k), (1, own_v)):
        @pl.when(z < nz - 1)
        def _():
            kv_copy(s, 0, 0, p, src).start()

        @pl.when(y == 0)
        def _():
            kv_copy(s, 1, 0, p, src).start()

    @pl.when(z > 0)
    def _():
        qg_copy(s, 0, 0, 0, own_q).start()

    @pl.when(y == 1)
    def _():
        qg_copy(s, 1, 0, 0, own_q).start()

    norm_backward(heads, width, lam, gain, mo, og, lse, own_g, col, row)

    @pl.when(z > 0)
    def _():
        st_copy(s, 0, 0, row).start()
        qg_copy(s, 0, 0, 1, own_g).start()

    @pl.when(y == 1)
    def _():
        st_copy(s, 1, 0, row).start()
        qg_copy(s, 1, 0, 1, own_g).start()

    lane_id = lax.broadcasted_iota(jnp.int32, (1, width), 1)
    low = jnp.where(lane_id < width // 2, 1.0, 0.0).astype(BF16)
    high = jnp.where(lane_id < width // 2, 0.0, 1.0).astype(BF16)

    def split(x):
        return jnp.concatenate([x * low, x * high], axis=0)

    def query_side(k_at, v_at, diagonal):
        def one(h, carry):
            at = pl.ds(pl.multiple_of(h * width, width), width)
            keys = split(k_at[:, at])
            scores = dot_nt(own_q[:, at], keys)
            mixed = dot_nt(own_g[:, at], v_at[:, at])
            stats = col[h]
            x1 = scores[:, :rows] * exp_scale - stats[:, 0:1]
            x2 = scores[:, rows:] * exp_scale - stats[:, 1:2]
            if diagonal:
                seen = (lax.broadcasted_iota(jnp.int32, (rows, rows), 1)
                        <= lax.broadcasted_iota(jnp.int32, (rows, rows), 0))
                x1 = jnp.where(seen, x1, -jnp.inf)
                x2 = jnp.where(seen, x2, -jnp.inf)
            g1 = (jnp.exp2(x1) * (mixed - stats[:, 2:3])).astype(BF16)
            g2 = (jnp.exp2(x2) * (stats[:, 3:4] - mixed)).astype(BF16)
            part_dq = dot_nn(jnp.concatenate([g1, g2], axis=1), keys)
            if diagonal:
                dq_acc[:, at] = part_dq
            else:
                dq_acc[:, at] += part_dq
            return carry
        lax.fori_loop(0, heads, one, 0)

    def key_side(q_at, g_at, row_at, diagonal):
        def one(h, carry):
            at = pl.ds(pl.multiple_of(h * width, width), width)
            queries = split(q_at[:, at])
            grads = g_at[:, at]
            scores = dot_nt(own_k[:, at], queries)
            mixed = dot_nt(own_v[:, at], grads)
            stats = row_at[h]
            x1 = scores[:, :rows] * exp_scale - stats[0:1]
            x2 = scores[:, rows:] * exp_scale - stats[1:2]
            if diagonal:
                seen = (lax.broadcasted_iota(jnp.int32, (rows, rows), 0)
                        <= lax.broadcasted_iota(jnp.int32, (rows, rows), 1))
                x1 = jnp.where(seen, x1, -jnp.inf)
                x2 = jnp.where(seen, x2, -jnp.inf)
            p1 = jnp.exp2(x1)
            p2 = jnp.exp2(x2)
            g1 = (p1 * (mixed - stats[2:3])).astype(BF16)
            g2 = (p2 * (stats[3:4] - mixed)).astype(BF16)
            part_dv = dot_nn((p1 - p2).astype(BF16), grads)
            part_dk = dot_nn(jnp.concatenate([g1, g2], axis=1), queries)
            if diagonal:
                dv_acc[:, at] = part_dv
                dk_acc[:, at] = part_dk
            else:
                dv_acc[:, at] += part_dv
                dk_acc[:, at] += part_dk
            return carry
        lax.fori_loop(0, heads, one, 0)

    def lat_copy(d):
        to = lax.rem(s + d, nsp)
        mine = pl.ds(pl.multiple_of(t * part, part), part)
        return copy(lat.at[mine, pl.ds(pl.multiple_of(to * slab, slab), slab)],
                    latb.at[s, mine, :], la_s.at[d], la_r.at[d], to)

    def own_lat():
        return pltpu.make_async_copy(
            lat.at[pl.ds(pl.multiple_of(t * part, part), part), pl.ds(pl.multiple_of(s * slab, slab), slab)],
            latb.at[s, pl.ds(pl.multiple_of(t * part, part), part), :], own_sem)

    def share_copy(d):
        mine = pl.ds(pl.multiple_of(t * part, part), part)
        return pltpu.make_async_remote_copy(
            src_ref=latb.at[:, mine, :], dst_ref=latb.at[:, mine, :],
            send_sem=lb_s.at[d], recv_sem=lb_r.at[d],
            device_id={"tp": lax.rem(t + d, ntp)}, device_id_type=MESH)

    own_lat().start()
    query_side(own_k, own_v, True)
    key_side(own_q, own_g, row, True)
    for d in range(1, nsp):
        lat_copy(d).start()

    def step(k, carry):
        below, above = z - k, z + k
        has_below, has_above = below >= 0, above < nz
        kb = jnp.maximum(below, 0) * 2 + y
        qb = jnp.minimum(above, nz - 1) * 2 + y

        for p in range(2):
            @pl.when(has_below)
            def _():
                kv_copy(kb, 0, 0, p).wait_recv()
                kv_copy(kb, 1, k, p).start()

            @pl.when(has_below & (z < nz - 1))
            def _():
                kv_copy(kb, 0, k, p).start()

            @pl.when(has_above)
            def _():
                qg_copy(qb, 0, 0, p).wait_recv()
                qg_copy(qb, 1, k, p).start()
                if p == 0:
                    st_copy(qb, 0, 0).wait_recv()
                    st_copy(qb, 1, k).start()

            @pl.when(has_above & (z > 0))
            def _():
                qg_copy(qb, 0, k, p).start()
                if p == 0:
                    st_copy(qb, 0, k).start()

        def turn(c, carry):
            dist = k - c
            other = jnp.where(c == 0, y, 1 - y)
            bz, qz = z - dist, z + dist
            use_kv = (bz >= 0) & (dist < nz) & ((dist > 0) | (y == 1))
            use_qg = (qz < nz) & (dist < nz) & ((dist > 0) | (y == 0))
            kblk = jnp.maximum(bz, 0) * 2 + other
            qblk = jnp.minimum(qz, nz - 1) * 2 + other

            @pl.when(use_kv)
            def _():
                @pl.when(c == 1)
                def _():
                    for p in range(2):
                        kv_copy(kblk, 1, 0, p).wait_recv()
                query_side(kvb.at[kblk, 0], kvb.at[kblk, 1], False)

            @pl.when(use_qg)
            def _():
                @pl.when(c == 1)
                def _():
                    for p in range(2):
                        qg_copy(qblk, 1, 0, p).wait_recv()
                    st_copy(qblk, 1, 0).wait_recv()
                key_side(qgb.at[qblk, 0], qgb.at[qblk, 1], stb.at[qblk], False)
            return carry
        lax.fori_loop(0, 2, turn, 0)
        return carry

    lax.fori_loop(1, nz + 1, step, 0)

    own_dq[...] = (dq_acc[...] * score_scale).astype(BF16)
    half = rows // 2

    def dq_copy(block, lane, idx, p, own=False):
        to = (jnp.minimum(s + 2, nsp - 2 + y), jnp.maximum(s - 2, y), side)[lane]
        at = pl.ds(p * half, half)
        return copy(own_dq.at[at] if own else dqb.at[block, at], dqb.at[block, at],
                    dq_s.at[lane, p, idx], dq_r.at[p, block], to)

    for p in range(2):
        @pl.when(z < nz - 1)
        def _():
            dq_copy(s, 0, z, p, True).start()

        @pl.when(z > 0)
        def _():
            dq_copy(s, 1, z, p, True).start()

        dq_copy(s, 2, z, p, True).start()

    for h in range(heads):
        at = slice(h * width, (h + 1) * width)
        dq_out[:, h, :] = own_dq[:, at]
        dk_out[:, h, :] = (dk_acc[:, at] * score_scale).astype(BF16)
        dv_out[:, h, :] = dv_acc[:, at].astype(BF16)

    own_lat().wait()
    for d in range(1, nsp):
        lat_copy(d).wait_recv()
    for d in range(1, ntp):
        share_copy(d).start()
    for d in range(1, ntp):
        share_copy(d).wait_recv()

    wg_out[...] = dot_tn(latb[s], own_dq[...])

    def add_block(block):
        wg_out[...] += dot_tn(latb[block], dqb[block])

    def gather(k, carry):
        for p in range(2):
            for lane, there, ok, more in (
                (0, z - k, z - k >= 0, z < nz - 1),
                (1, z + k, z + k < nz, z > 0),
            ):
                bz = jnp.clip(there, 0, nz - 1)
                block = bz * 2 + y

                @pl.when(ok)
                def _():
                    dq_copy(block, lane, bz, p).wait_recv()
                    dq_copy(block, 2, bz, p).start()

                @pl.when(ok & more)
                def _():
                    dq_copy(block, lane, bz, p).start()

        def turn(c, carry):
            dist = jnp.where(c < 2, k, k - 1)
            up = lax.rem(c, 2)
            bz = jnp.where(up == 0, z - dist, z + dist)
            ok = (bz >= 0) & (bz < nz) & (dist < nz) & ((dist > 0) | (up == 0))
            other = jnp.where(c < 2, y, 1 - y)
            block = jnp.clip(bz, 0, nz - 1) * 2 + other

            @pl.when(ok)
            def _():
                @pl.when(c >= 2)
                def _():
                    for p in range(2):
                        dq_copy(block, 2, 0, p).wait_recv()
                add_block(block)
            return carry
        lax.fori_loop(0, 4, turn, 0)
        return carry

    lax.fori_loop(1, nz + 1, gather, 0)

    def drain(k, carry):
        below, above = z - k, z + k
        has_below, has_above = below >= 0, above < nz

        for p in range(2):
            @pl.when(has_below & (z < nz - 1))
            def _():
                kv_copy(s, 0, k, p).wait_send()

            @pl.when(has_below & ((k > 0) | (y == 0)))
            def _():
                kv_copy(s, 1, k, p).wait_send()

            @pl.when(has_above & (z > 0))
            def _():
                qg_copy(s, 0, k, p).wait_send()
                if p == 0:
                    st_copy(s, 0, k).wait_send()

            @pl.when(has_above & ((k > 0) | (y == 1)))
            def _():
                qg_copy(s, 1, k, p).wait_send()
                if p == 0:
                    st_copy(s, 1, k).wait_send()

            @pl.when((k <= z) & (z < nz - 1))
            def _():
                dq_copy(s, 0, k, p).wait_send()

            @pl.when((k >= z) & (z > 0))
            def _():
                dq_copy(s, 1, k, p).wait_send()

            dq_copy(s, 2, k, p).wait_send()
        return carry

    lax.fori_loop(0, nz, drain, 0)
    for d in range(1, nsp):
        lat_copy(d).wait_send()
    for d in range(1, ntp):
        share_copy(d).wait_send()


def vmem():
    return pl.BlockSpec(memory_space=pltpu.VMEM)


def body(nsp, ntp, latents, query_heads, key_heads, value_heads, map_outputs, log_sums, out_grad,
         mix_lambda, norm_gain):
    rows, heads, width = query_heads.shape
    flat = (rows, heads * width)
    slab = latents.shape[1] // nsp
    nz = nsp // 2
    dma = pltpu.SemaphoreType.DMA
    dq, dk, dv, wg = pl.pallas_call(
        functools.partial(main_kernel, nsp, ntp, heads, width),
        out_shape=(
            jax.ShapeDtypeStruct(query_heads.shape, BF16),
            jax.ShapeDtypeStruct(query_heads.shape, BF16),
            jax.ShapeDtypeStruct(query_heads.shape, BF16),
            jax.ShapeDtypeStruct((slab, heads * width), F32),
        ),
        in_specs=[pl.BlockSpec(memory_space=pltpu.SMEM)] + [vmem()] * 8,
        out_specs=(vmem(),) * 4,
        scratch_shapes=[
            pltpu.VMEM(flat, BF16),
            pltpu.VMEM((heads, rows, width), F32),
            pltpu.VMEM((heads, 4, rows), F32),
            pltpu.VMEM(flat, BF16),
            pltpu.VMEM((nsp, 2) + flat, BF16),
            pltpu.VMEM((nsp, 2) + flat, BF16),
            pltpu.VMEM((nsp, heads, 4, rows), F32),
            pltpu.VMEM((nsp,) + flat, BF16),
            pltpu.VMEM((nsp, rows, slab), BF16),
            pltpu.VMEM(flat, F32),
            pltpu.VMEM(flat, F32),
            pltpu.VMEM(flat, F32),
            dma((2, 2, nz)), dma((2, 2, nz)), dma((2, nz)), dma((3, 2, nz)),
            dma((2, nsp)), dma((2, nsp)), dma((nsp,)), dma((2, nsp)),
            dma((nsp,)), dma((nsp,)), dma((ntp,)), dma((ntp,)),
            dma,
        ],
        compiler_params=pltpu.CompilerParams(collective_id=0, has_side_effects=True),
        name="main",
    )(
        mix_lambda,
        norm_gain[None, :],
        latents,
        key_heads.reshape(flat),
        value_heads.reshape(flat),
        query_heads.reshape(flat),
        map_outputs,
        out_grad,
        jnp.transpose(log_sums, (1, 0, 2)),
    )
    return dq, dk, dv, wg


def solution(mesh):
    placed = (
        P("sp", None),
        P("sp", "tp", None),
        P("sp", "tp", None),
        P("sp", "tp", None),
        P("sp", None, "tp", None),
        P("sp", "tp", None),
        P("sp", "tp", None),
        P("tp"),
        P(),
    )
    return jax.shard_map(
        functools.partial(body, mesh.shape["sp"], mesh.shape["tp"]),
        mesh=mesh,
        in_specs=placed,
        out_specs=(P("sp", "tp", None), P("sp", "tp", None), P("sp", "tp", None), P("sp", "tp")),
        check_vma=False,
    )
```
